32 devices in a mesh: gr: 2 (over x), fs: 8 (over z, y), tp: 2 (over core).
Axes of the slice: x: 2, y: 2, z: 4, core: 2. Of those that a mesh axis runs over, the one named last changes fastest.
Arguments:
- tokens: bfloat16 [2048, 2048], P(('gr', 'tp')), may hold values from -6 to 6
- norm_gain: float32 [2048], P('fs'), may hold values from 0.1 to 1.9
- up_weight: float32 [2048, 8192], P('fs', ('gr', 'tp')), may hold values from -0.125 to 0.125
- down_weight: float32 [8192, 2048], P('fs', ('gr', 'tp')), may hold values from -0.09375 to 0.09375
Outputs:
- sampler_up: bfloat16 [2048, 8192], P(None, 'fs')
- sampler_down: bfloat16 [8192, 2048], P('fs')
- mixed: bfloat16 [2048, 2048], P(('gr', 'tp'), 'fs')
The draws below stay inside these ranges and needn't reach their ends.
All inputs are finite; a program needn't handle non-finite values.
Results may differ from the reference program's by a relative error of at most 0.023.
Values may be sent and summed in bfloat16 or wider, within the bound.
A program may use at most 64 MiB of HBM per device.

```python
import jax
import jax.numpy as jnp
from jax import lax

D = 2048
FF = 8192
ROWS = 2048
N_FS = 8


def spiked(drawn, stream_key, source, target, blocks, factor):
    owner, partner = [(jnp.arange(drawn.shape[position]) // (drawn.shape[position] // blocks)).reshape([-1 if axis == position else 1 for axis in range(drawn.ndim)]) for position in (source, target)]
    chosen = jax.random.permutation(stream_key, blocks)[partner]
    strong = (owner == chosen) | (owner == (partner + blocks // 2) % blocks)
    return jnp.where(strong, factor * drawn, drawn)


def block_levels(rng, shape, cuts, smallest, top_value):
    gain, own = 1.0, jax.random.fold_in(rng, 6)
    for axis_at, blocks in cuts:
        draws = jnp.exp(jax.random.uniform(jax.random.fold_in(own, axis_at), (blocks,), jnp.float32, smallest / len(cuts), top_value / len(cuts)))
        gain = gain * jnp.repeat(draws, shape[axis_at] // blocks).reshape([-1 if axis == axis_at else 1 for axis in range(len(shape))])
    return gain


def bell_draw(key, extent, deviation, bound, cuts=(), held_as=jnp.bfloat16):
    result = jax.random.normal(key, extent, jnp.float32) * deviation
    if len(cuts) > 0:
        result = block_levels(key, extent, cuts, -0.22, 0.18) * result
    return jnp.clip(result, min=-bound, max=bound).astype(held_as)


def heavy_noise(own_key, dims, spread, limit, shards, heavy, held_as=jnp.bfloat16):
    entries = spread * jax.random.normal(own_key, dims, jnp.float32)
    if shards:
        entries = entries * block_levels(own_key, dims, shards, -0.22, 0.18)
    return jnp.clip(spiked(entries, jax.random.fold_in(own_key, 3), *heavy), -limit, limit).astype(held_as)


def setup_inputs(seed: int = 0) -> dict:
    streams_of = jax.random.split(jax.random.key(seed), 5)
    tokens = bell_draw(streams_of[0], (ROWS, D), 1.0, 6.0, ((0, 4),))
    norm_gain = jnp.clip(1.0 + 0.18 * jax.random.normal(streams_of[1], (D,), jnp.float32), 0.1, 1.9)
    up_weight = bell_draw(streams_of[2], (D, FF), D ** -0.5, 0.125, ((0, 8), (1, 4)), jnp.float32)
    down_weight = heavy_noise(streams_of[3], (FF, D), FF ** -0.5, 0.09375, ((0, 8), (1, 4)), (0, 1, 8, 2.0), jnp.float32)
    return dict(tokens=tokens, norm_gain=norm_gain, up_weight=up_weight, down_weight=down_weight)


def reference(tokens, norm_gain, up_weight, down_weight):
    sampler_up = (norm_gain[:, None] * up_weight).astype(jnp.bfloat16)
    sampler_down = down_weight.astype(jnp.bfloat16)
    widened = tokens.astype(jnp.float32)
    normed = (widened * lax.rsqrt(lax.optimization_barrier(jnp.mean(widened * widened, axis=-1, keepdims=True)) + 1e-06)).astype(jnp.bfloat16)
    preact = jnp.dot(normed, sampler_up, preferred_element_type=jnp.float32)
    hidden = jnp.square(jax.nn.relu(preact)).astype(jnp.bfloat16)
    block_units = FF // N_FS

    def add_block(total, index):
        begin = (index * block_units).astype(jnp.int32)
        hidden_part = lax.dynamic_slice_in_dim(hidden, begin, block_units, 1)
        down_part = lax.dynamic_slice_in_dim(sampler_down, begin, block_units, 0)
        partial_value = jnp.dot(hidden_part, down_part, preferred_element_type=jnp.float32).astype(jnp.bfloat16)
        partial_value = lax.optimization_barrier(partial_value)
        return (total + partial_value.astype(jnp.float32), None)
    start_total = jnp.zeros((tokens.shape[0], D), jnp.float32)
    summed, _ = lax.scan(add_block, start_total, jnp.arange(N_FS, dtype=jnp.int32))
    return (sampler_up, sampler_down, summed.astype(jnp.bfloat16))
```

```python
import functools

import jax
import jax.numpy as jnp
from jax import lax
from jax.experimental import pallas as pl
from jax.experimental.pallas import tpu as pltpu
from jax.sharding import PartitionSpec as P

MESH = pl.DeviceIdType.MESH
VMEM_LIMIT = 60 * 1024 * 1024


def flipped(index, step, count):
    if count & (count - 1):
        return lax.rem(index + step, count)
    bit = 1
    while bit < count:
        if step & bit:
            index = index + (1 - 2 * lax.rem(index // bit, 2)) * bit
        bit *= 2
    return index


def remote(src, dst, send, recv, device):
    return pltpu.make_async_remote_copy(
        src_ref=src, dst_ref=dst, send_sem=send, recv_sem=recv,
        device_id=device, device_id_type=MESH,
    )


def gather_kernel(
    tp, blocks, shards, tokens, gain, up, down, up_out, down_out, hidden_out,
    gath, normed, acc, xs, xr, fsend, frecv, ps, pr, ds_, dr, pds, pdr,
):
    g, f, t = lax.axis_index("gr"), lax.axis_index("fs"), lax.axis_index("tp")
    per = tp // 2
    chips = gath.shape[0]
    c, k = g * per + t // 2, lax.rem(t, 2)
    rows, width = up.shape
    half = rows // 2
    block = width // blocks
    cols = down.shape[1]

    def dev(chip, shard, core):
        return (chip // per, shard, lax.rem(chip, per) * 2 + core)

    def down_cols(chip, core):
        return pl.ds(pl.multiple_of((chip * 2 + core) * cols, cols), cols)

    barrier = pltpu.get_barrier_semaphore()
    for s in range(1, chips):
        pl.semaphore_signal(
            barrier, inc=1, device_id=dev(lax.rem(c + s, chips), f, k), device_id_type=MESH
        )
    for s in range(shards):
        for core in range(2):
            if s == 0 and core == 0:
                continue
            other = lax.rem(f + s, shards)
            core_id = lax.rem(k + core, 2)
            pl.semaphore_signal(
                barrier, inc=1, device_id=dev(c, other, core_id), device_id_type=MESH
            )

    gath[c] = (gain[...] * up[...]).astype(jnp.bfloat16)
    down_out[:, down_cols(c, k)] = down[...].astype(jnp.bfloat16)
    pl.semaphore_wait(barrier, chips - 1 + 2 * shards - 1)

    def unit(chip, j, h):
        return gath.at[chip, pl.ds(h * half, half), pl.ds(j * block, block)]

    def up_rows(shard, core):
        return up_out.at[pl.ds(pl.multiple_of(shard * rows + core * half, half), half), :]

    def target(chip, j):
        return (chip * 2 + k) * blocks + j

    def forward(chip, j, h):
        to = target(chip, j)
        return remote(
            unit(chip, j, h), up_rows(f, h), fsend.at[chip, j, h], frecv.at[f], dev(c, to, h)
        )

    def stays(chip, j, h):
        return jnp.logical_and(target(chip, j) == f, k == h)

    def start_forward(chip, j, h):
        @pl.when(jnp.logical_not(stays(chip, j, h)))
        def _():
            forward(chip, j, h).start()

        @pl.when(stays(chip, j, h))
        def _():
            up_rows(f, h)[...] = unit(chip, j, h)[...]

    def exchange(s, j, h):
        return remote(
            unit(c, j, h), unit(c, j, h), xs.at[s, j, h], xr.at[s, j, h],
            dev(lax.rem(c + s, chips), f, k),
        )

    def exchanged(s, j, h):
        source = lax.rem(c + chips - s, chips)
        return remote(
            unit(source, j, h), unit(source, j, h), xs.at[s, j, h], xr.at[s, j, h], dev(c, f, k)
        )

    def down_copy(s):
        mine = down_out.at[:, down_cols(c, k)]
        return remote(mine, mine, ds_.at[s], dr.at[s], dev(lax.rem(c + s, chips), f, k))

    def down_relay(s, core):
        held = down_out.at[:, down_cols(lax.rem(c + chips - s, chips), core)]
        return remote(held, held, pds.at[s], pdr.at[s], dev(c, f, 1 - k))

    units = [(j, h) for h in range(2) for j in range(blocks)]
    for j, h in units:
        for s in range(1, chips):
            exchange(s, j, h).start()
        start_forward(c, j, h)
    for s in range(1, chips):
        down_copy(s).start()
    down_relay(0, k).start()

    widened = tokens[...].astype(jnp.float32)
    scale = lax.rsqrt(jnp.mean(widened * widened, axis=-1, keepdims=True) + 1e-06)
    for shard in range(shards):
        part = tokens[:, shard * rows:(shard + 1) * rows].astype(jnp.float32)
        normed[shard] = (part * scale).astype(jnp.bfloat16)

    for j, h in units:
        for s in range(1, chips):
            exchanged(s, j, h).wait_recv()
            start_forward(lax.rem(c + chips - s, chips), j, h)

    source_core = lax.rem(f // blocks, 2)
    own_stays = source_core == k

    def arrival(shard):
        return remote(
            up_rows(shard, k), up_rows(shard, k), ps.at[shard], frecv.at[shard], dev(c, f, 1 - k)
        )

    def relay(shard, core):
        held = up_rows(shard, core)
        return remote(held, held, ps.at[shard], pr.at[shard], dev(c, f, 1 - k))

    def accumulate(shard, first):
        weights = up_out[pl.ds(pl.multiple_of(shard * rows, rows), rows), :]
        product = jnp.dot(normed[shard], weights, preferred_element_type=jnp.float32)
        if first:
            acc[...] = product
        else:
            acc[...] += product

    order = [flipped(f, s, shards) for s in list(range(1, shards)) + [0]]
    for position, shard in enumerate(order):
        if position < shards - 1:
            arrival(shard).wait_recv()
        else:
            @pl.when(jnp.logical_not(own_stays))
            def _():
                arrival(shard).wait_recv()
        relay(shard, k).start()
        if position > 0:
            before = order[position - 1]
            relay(before, 1 - k).wait_recv()
            accumulate(before, position == 1)
    for s in range(1, chips):
        down_copy_in = remote(
            down_out.at[:, down_cols(lax.rem(c + chips - s, chips), k)],
            down_out.at[:, down_cols(lax.rem(c + chips - s, chips), k)],
            ds_.at[s], dr.at[s], dev(c, f, 1 - k),
        )
        down_copy_in.wait_recv()
        down_relay(s, k).start()
    relay(order[-1], 1 - k).wait_recv()
    accumulate(order[-1], False)
    hidden_out[...] = jnp.square(jnp.maximum(acc[...], 0.0)).astype(jnp.bfloat16)

    for s in range(chips):
        down_relay(s, 1 - k).wait_recv()
        down_relay(s, k).wait_send()
    for s in range(1, chips):
        down_copy(s).wait_send()
        for j, h in units:
            exchange(s, j, h).wait_send()
    for shard in order:
        relay(shard, k).wait_send()
    for s in range(chips):
        chip = lax.rem(c + s, chips)
        for j, h in units:
            @pl.when(jnp.logical_not(stays(chip, j, h)))
            def _():
                forward(chip, j, h).wait_send()


def reduce_kernel(hidden, down, mixed, part, ybuf, zout, zbuf, ys, yr, zs, zr):
    g, f, t = lax.axis_index("gr"), lax.axis_index("fs"), lax.axis_index("tp")
    pairs = ybuf.shape[0]
    wide = mixed.shape[1]
    z, y = f // 2, lax.rem(f, 2)

    barrier = pltpu.get_barrier_semaphore()
    pl.semaphore_signal(
        barrier, inc=1, device_id=(g, z * 2 + 1 - y, t), device_id_type=MESH
    )
    for s in range(1, pairs):
        pl.semaphore_signal(
            barrier, inc=1, device_id=(g, lax.rem(z + s, pairs) * 2 + y, t), device_id_type=MESH
        )
    order = [flipped(z, s, pairs) for s in list(range(pairs - 1, 0, -1)) + [0]]

    def compute(pair):
        columns = pl.ds(pl.multiple_of(pair * 2 * wide, 2 * wide), 2 * wide)
        both = jnp.dot(hidden[...], down[:, columns], preferred_element_type=jnp.float32)
        both = both.astype(jnp.bfloat16)
        part[2 * pair] = both[:, :wide]
        part[2 * pair + 1] = both[:, wide:]

    def across(pair):
        return remote(
            part.at[2 * pair + 1 - y], ybuf.at[pair], ys.at[pair], yr.at[pair],
            (g, z * 2 + 1 - y, t),
        )

    def along(pair, sender):
        return remote(
            zout.at[pair], zbuf.at[sender], zs.at[pair], zr.at[sender], (g, pair * 2 + y, t)
        )

    compute(order[0])
    pl.semaphore_wait(barrier, pairs)
    for position in range(1, pairs):
        compute(order[position])
        across(order[position - 1]).start()
    across(order[-1]).start()

    previous = None
    for pair in order[:-1]:
        across(pair).wait_recv()
        zout[pair] = (
            part[2 * pair + y].astype(jnp.float32) + ybuf[pair].astype(jnp.float32)
        ).astype(jnp.bfloat16)
        along(pair, z).start()
    across(order[-1]).wait_recv()
    total = part[2 * z + y].astype(jnp.float32) + ybuf[z].astype(jnp.float32)
    for pair in order[-2::-1]:
        along(z, pair).wait_recv()
        total = total + zbuf[pair].astype(jnp.float32)
    mixed[...] = total.astype(jnp.bfloat16)
    for pair in order:
        across(pair).wait_send()
    for pair in order[:-1]:
        along(pair, z).wait_send()


def per_device(gr, fs, tp, tokens, norm_gain, up_weight, down_weight):
    rows, width = up_weight.shape
    units, cols = down_weight.shape
    group = gr * tp
    chips = group // 2
    block = width * group // fs
    blocks = width // block
    count, depth = tokens.shape
    model = cols * group
    vmem = pl.BlockSpec(memory_space=pltpu.VMEM)
    bf16, f32 = jnp.bfloat16, jnp.float32
    dma = pltpu.SemaphoreType.DMA
    up_block, down_columns, hidden = pl.pallas_call(
        functools.partial(gather_kernel, tp, blocks, fs),
        out_shape=(
            jax.ShapeDtypeStruct((depth, block), bf16),
            jax.ShapeDtypeStruct((units, model), bf16),
            jax.ShapeDtypeStruct((count, block), bf16),
        ),
        in_specs=[vmem] * 4,
        out_specs=(vmem,) * 3,
        scratch_shapes=[
            pltpu.VMEM((chips, rows, width), bf16),
            pltpu.VMEM((fs, count, rows), bf16),
            pltpu.VMEM((count, block), f32),
            dma((chips, blocks, 2)), dma((chips, blocks, 2)),
            dma((chips, blocks, 2)), dma((fs,)),
            dma((fs,)), dma((fs,)),
            dma((chips,)), dma((chips,)), dma((chips,)), dma((chips,)),
        ],
        compiler_params=pltpu.CompilerParams(
            collective_id=0, has_side_effects=True, vmem_limit_bytes=VMEM_LIMIT
        ),
    )(tokens, norm_gain[:, None], up_weight, down_weight)
    pairs = fs // 2
    wide = model // fs
    mixed = pl.pallas_call(
        reduce_kernel,
        out_shape=jax.ShapeDtypeStruct((count, wide), bf16),
        in_specs=[vmem] * 2,
        out_specs=vmem,
        scratch_shapes=[
            pltpu.VMEM((fs, count, wide), bf16),
            pltpu.VMEM((pairs, count, wide), bf16),
            pltpu.VMEM((pairs, count, wide), bf16),
            pltpu.VMEM((pairs, count, wide), bf16),
            dma((pairs,)), dma((pairs,)), dma((pairs,)), dma((pairs,)),
        ],
        compiler_params=pltpu.CompilerParams(
            collective_id=1, has_side_effects=True, vmem_limit_bytes=VMEM_LIMIT
        ),
    )(hidden, down_columns)
    return (up_block, down_columns, mixed)


def solution(mesh):
    in_specs = (P(("gr", "tp"), None), P("fs"), P("fs", ("gr", "tp")), P("fs", ("gr", "tp")))
    out_specs = (P(None, "fs"), P("fs", None), P(("gr", "tp"), "fs"))
    body = functools.partial(per_device, mesh.shape["gr"], mesh.shape["fs"], mesh.shape["tp"])
    return jax.shard_map(
        body, mesh=mesh, in_specs=in_specs, out_specs=out_specs, check_vma=False
    )
```

```python
import functools

import jax
import jax.numpy as jnp
from jax import lax
from jax.experimental import pallas as pl
from jax.experimental.pallas import tpu as pltpu
from jax.sharding import PartitionSpec as P

MESH = pl.DeviceIdType.MESH
MIB = 1024 * 1024
GATHER_VMEM = 32
REDUCE_VMEM = 20
SLICES = 2
PIECES = 2


def flipped(index, step, count):
    if count & (count - 1):
        return lax.rem(index + step, count)
    bit = 1
    while bit < count:
        if step & bit:
            index = index + (1 - 2 * lax.rem(index // bit, 2)) * bit
        bit *= 2
    return index


def remote(src, dst, send, recv, device):
    return pltpu.make_async_remote_copy(
        src_ref=src, dst_ref=dst, send_sem=send, recv_sem=recv,
        device_id=device, device_id_type=MESH,
    )


def gather_kernel(
    tp, blocks, shards, tokens, gain, up, down, up_out, down_out, hidden_out,
    gath, normed, acc, xs, xr, fsend, frecv, ps, pr, ds_, dr, pds, pdr,
):
    g, f, t = lax.axis_index("gr"), lax.axis_index("fs"), lax.axis_index("tp")
    per = tp // 2
    chips = gath.shape[0]
    c, k = g * per + t // 2, lax.rem(t, 2)
    rows, width = up.shape
    half = rows // 2
    block = width // blocks
    cols = down.shape[1]

    def dev(chip, shard, core):
        return (chip // per, shard, lax.rem(chip, per) * 2 + core)

    def down_cols(chip, core):
        return pl.ds(pl.multiple_of((chip * 2 + core) * cols, cols), cols)

    barrier = pltpu.get_barrier_semaphore()
    for s in range(1, chips):
        pl.semaphore_signal(
            barrier, inc=1, device_id=dev(lax.rem(c + s, chips), f, k), device_id_type=MESH
        )
    for s in range(shards):
        for core in range(2):
            if s == 0 and core == 0:
                continue
            other = lax.rem(f + s, shards)
            core_id = lax.rem(k + core, 2)
            pl.semaphore_signal(
                barrier, inc=1, device_id=dev(c, other, core_id), device_id_type=MESH
            )

    square = (rows, rows)
    diagonal = lax.broadcasted_iota(jnp.int32, square, 0) == lax.broadcasted_iota(jnp.int32, square, 1)
    column = jnp.sum(jnp.where(diagonal, gain[...], 0.0), axis=1, keepdims=True)
    gath[c] = (column * up[...]).astype(jnp.bfloat16)
    down_out[:, down_cols(c, k)] = down[...].astype(jnp.bfloat16)
    pl.semaphore_wait(barrier, chips - 1 + 2 * shards - 1)

    slices = xs.shape[2] // 2
    piece = half // slices

    def unit(chip, j, u):
        return gath.at[chip, pl.ds(u * piece, piece), pl.ds(j * block, block)]

    def up_rows(shard, core):
        return up_out.at[pl.ds(pl.multiple_of(shard * rows + core * half, half), half), :]

    def target(chip, j):
        return (chip * 2 + k) * blocks + j

    def landing(u):
        return up_out.at[pl.ds(pl.multiple_of(f * rows + u * piece, piece), piece), :]

    def forward(chip, j, u):
        to = target(chip, j)
        return remote(
            unit(chip, j, u), landing(u), fsend.at[chip, j, u], frecv.at[f],
            dev(c, to, u // slices),
        )

    def stays(chip, j, u):
        return jnp.logical_and(target(chip, j) == f, k == u // slices)

    def start_forward(chip, j, h):
        @pl.when(jnp.logical_not(stays(chip, j, h)))
        def _():
            forward(chip, j, h).start()

        @pl.when(stays(chip, j, h))
        def _():
            landing(h)[...] = unit(chip, j, h)[...]

    def exchange(s, j, h):
        return remote(
            unit(c, j, h), unit(c, j, h), xs.at[s, j, h], xr.at[s, j, h],
            dev(lax.rem(c + s, chips), f, k),
        )

    def exchanged(s, j, h):
        source = lax.rem(c + chips - s, chips)
        return remote(
            unit(source, j, h), unit(source, j, h), xs.at[s, j, h], xr.at[s, j, h], dev(c, f, k)
        )

    def down_copy(s):
        mine = down_out.at[:, down_cols(c, k)]
        return remote(mine, mine, ds_.at[s], dr.at[s], dev(lax.rem(c + s, chips), f, k))

    def down_relay(s, core):
        held = down_out.at[:, down_cols(lax.rem(c + chips - s, chips), core)]
        return remote(held, held, pds.at[s], pdr.at[s], dev(c, f, 1 - k))

    units = [(j, q + core * slices) for q in range(slices) for core in range(2) for j in range(blocks)]
    for j, h in units:
        for s in range(1, chips):
            exchange(s, j, h).start()
        start_forward(c, j, h)
    for s in range(1, chips):
        down_copy(s).start()
    down_relay(0, k).start()

    widened = tokens[...].astype(jnp.float32)
    scale = lax.rsqrt(jnp.mean(widened * widened, axis=-1, keepdims=True) + 1e-06)
    for shard in range(shards):
        part = tokens[:, shard * rows:(shard + 1) * rows].astype(jnp.float32)
        normed[shard] = (part * scale).astype(jnp.bfloat16)

    for j, h in units:
        for s in range(1, chips):
            exchanged(s, j, h).wait_recv()
            start_forward(lax.rem(c + chips - s, chips), j, h)

    source_core = lax.rem(f // blocks, 2)
    own_stays = source_core == k

    def arrival(shard):
        return remote(
            up_rows(shard, k), up_rows(shard, k), ps.at[shard], frecv.at[shard], dev(c, f, 1 - k)
        )

    def relay(shard, core):
        held = up_rows(shard, core)
        return remote(held, held, ps.at[shard], pr.at[shard], dev(c, f, 1 - k))

    def accumulate(shard, first):
        weights = up_out[pl.ds(pl.multiple_of(shard * rows, rows), rows), :]
        product = jnp.dot(normed[shard], weights, preferred_element_type=jnp.float32)
        if first:
            acc[...] = product
        else:
            acc[...] += product

    order = [flipped(f, s, shards) for s in list(range(1, shards)) + [0]]
    for position, shard in enumerate(order):
        if position < shards - 1:
            arrival(shard).wait_recv()
        else:
            @pl.when(jnp.logical_not(own_stays))
            def _():
                arrival(shard).wait_recv()
        relay(shard, k).start()
        if position > 0:
            before = order[position - 1]
            relay(before, 1 - k).wait_recv()
            accumulate(before, position == 1)
    for s in range(1, chips):
        down_copy_in = remote(
            down_out.at[:, down_cols(lax.rem(c + chips - s, chips), k)],
            down_out.at[:, down_cols(lax.rem(c + chips - s, chips), k)],
            ds_.at[s], dr.at[s], dev(c, f, 1 - k),
        )
        down_copy_in.wait_recv()
        down_relay(s, k).start()
    relay(order[-1], 1 - k).wait_recv()
    accumulate(order[-1], False)
    hidden_out[...] = jnp.square(jnp.maximum(acc[...], 0.0)).astype(jnp.bfloat16)

    for s in range(chips):
        down_relay(s, 1 - k).wait_recv()
        down_relay(s, k).wait_send()
    for s in range(1, chips):
        down_copy(s).wait_send()
        for j, h in units:
            exchange(s, j, h).wait_send()
    for shard in order:
        relay(shard, k).wait_send()
    for s in range(chips):
        chip = lax.rem(c + s, chips)
        for j, h in units:
            @pl.when(jnp.logical_not(stays(chip, j, h)))
            def _():
                forward(chip, j, h).wait_send()


def reduce_kernel(hidden, down, mixed, part, ybuf, zout, zbuf, ys, yr, zs, zr):
    g, f, t = lax.axis_index("gr"), lax.axis_index("fs"), lax.axis_index("tp")
    pairs = ybuf.shape[0]
    wide = mixed.shape[1]
    z, y = f // 2, lax.rem(f, 2)

    barrier = pltpu.get_barrier_semaphore()
    pl.semaphore_signal(
        barrier, inc=1, device_id=(g, z * 2 + 1 - y, t), device_id_type=MESH
    )
    for s in range(1, pairs):
        pl.semaphore_signal(
            barrier, inc=1, device_id=(g, lax.rem(z + s, pairs) * 2 + y, t), device_id_type=MESH
        )
    order = [flipped(z, s, pairs) for s in list(range(pairs - 1, 0, -1)) + [0]]

    def compute(pair):
        columns = pl.ds(pl.multiple_of(pair * 2 * wide, 2 * wide), 2 * wide)
        both = jnp.dot(hidden[...], down[:, columns], preferred_element_type=jnp.float32)
        both = both.astype(jnp.bfloat16)
        part[2 * pair] = both[:, :wide]
        part[2 * pair + 1] = both[:, wide:]

    pieces = ys.shape[1]
    span = mixed.shape[0] // pieces

    def across(pair, i):
        tokens = pl.ds(i * span, span)
        return remote(
            part.at[2 * pair + 1 - y, tokens], ybuf.at[pair, tokens], ys.at[pair, i],
            yr.at[pair, i], (g, z * 2 + 1 - y, t),
        )

    def along(pair, sender, i):
        tokens = pl.ds(i * span, span)
        return remote(
            zout.at[pair, tokens], zbuf.at[sender, tokens], zs.at[pair, i], zr.at[sender, i],
            (g, pair * 2 + y, t),
        )

    compute(order[0])
    pl.semaphore_wait(barrier, pairs)
    for position in range(1, pairs + 1):
        if position < pairs:
            compute(order[position])
        for i in range(pieces):
            across(order[position - 1], i).start()

    def summed(pair, i):
        tokens = pl.ds(i * span, span)
        return part[2 * pair + y, tokens].astype(jnp.float32) + ybuf[pair, tokens].astype(jnp.float32)

    for pair in order[:-1]:
        for i in range(pieces):
            across(pair, i).wait_recv()
            zout[pair, pl.ds(i * span, span)] = summed(pair, i).astype(jnp.bfloat16)
            along(pair, z, i).start()
    for i in range(pieces):
        tokens = pl.ds(i * span, span)
        across(z, i).wait_recv()
        total = summed(z, i)
        for pair in order[:-1]:
            along(z, pair, i).wait_recv()
            total = total + zbuf[pair, tokens].astype(jnp.float32)
        mixed[tokens] = total.astype(jnp.bfloat16)
    for i in range(pieces):
        for pair in order:
            across(pair, i).wait_send()
        for pair in order[:-1]:
            along(pair, z, i).wait_send()


def per_device(gr, fs, tp, tokens, norm_gain, up_weight, down_weight):
    rows, width = up_weight.shape
    units, cols = down_weight.shape
    group = gr * tp
    chips = group // 2
    block = width * group // fs
    blocks = width // block
    count, depth = tokens.shape
    model = cols * group
    vmem = pl.BlockSpec(memory_space=pltpu.VMEM)
    bf16, f32 = jnp.bfloat16, jnp.float32
    dma = pltpu.SemaphoreType.DMA
    up_block, down_columns, hidden = pl.pallas_call(
        functools.partial(gather_kernel, tp, blocks, fs),
        out_shape=(
            jax.ShapeDtypeStruct((depth, block), bf16),
            jax.ShapeDtypeStruct((units, model), bf16),
            jax.ShapeDtypeStruct((count, block), bf16),
        ),
        in_specs=[vmem] * 4,
        out_specs=(vmem,) * 3,
        scratch_shapes=[
            pltpu.VMEM((chips, rows, width), bf16),
            pltpu.VMEM((fs, count, rows), bf16),
            pltpu.VMEM((count, block), f32),
            *[dma((chips, blocks, 2 * SLICES)) for _ in range(3)], dma((fs,)),
            dma((fs,)), dma((fs,)),
            dma((chips,)), dma((chips,)), dma((chips,)), dma((chips,)),
        ],
        compiler_params=pltpu.CompilerParams(
            collective_id=0, has_side_effects=True, vmem_limit_bytes=GATHER_VMEM * MIB
        ),
        cost_estimate=pl.CostEstimate(
            flops=2 * count * depth * block, bytes_accessed=160 * MIB, transcendentals=0
        ),
    )(tokens, norm_gain[None, :], up_weight, down_weight)
    pairs = fs // 2
    wide = model // fs
    mixed = pl.pallas_call(
        reduce_kernel,
        out_shape=jax.ShapeDtypeStruct((count, wide), bf16),
        in_specs=[vmem] * 2,
        out_specs=vmem,
        scratch_shapes=[
            pltpu.VMEM((fs, count, wide), bf16),
            pltpu.VMEM((pairs, count, wide), bf16),
            pltpu.VMEM((pairs, count, wide), bf16),
            pltpu.VMEM((pairs, count, wide), bf16),
            *[dma((pairs, PIECES)) for _ in range(4)],
        ],
        compiler_params=pltpu.CompilerParams(
            collective_id=1, has_side_effects=True, vmem_limit_bytes=REDUCE_VMEM * MIB
        ),
        cost_estimate=pl.CostEstimate(
            flops=2 * count * units * model, bytes_accessed=100 * MIB, transcendentals=0
        ),
    )(hidden, down_columns)
    return (up_block, down_columns, mixed)


def solution(mesh):
    in_specs = (P(("gr", "tp"), None), P("fs"), P("fs", ("gr", "tp")), P("fs", ("gr", "tp")))
    out_specs = (P(None, "fs"), P("fs", None), P(("gr", "tp"), "fs"))
    body = functools.partial(per_device, mesh.shape["gr"], mesh.shape["fs"], mesh.shape["tp"])
    return jax.shard_map(
        body, mesh=mesh, in_specs=in_specs, out_specs=out_specs, check_vma=False
    )
```

```python
import functools

import jax
import jax.numpy as jnp
from jax import lax
from jax.experimental import pallas as pl
from jax.experimental.pallas import tpu as pltpu
from jax.sharding import PartitionSpec as P

MESH = pl.DeviceIdType.MESH
MIB = 1024 * 1024
GATHER_VMEM = 32
PARTIAL_VMEM = 20
REDUCE_VMEM = 20
SLICE_ROWS = 32
PIECES = 2


def flipped(index, step, count):
    if count & (count - 1):
        return lax.rem(index + step, count)
    bit = 1
    while bit < count:
        if step & bit:
            index = index + (1 - 2 * lax.rem(index // bit, 2)) * bit
        bit *= 2
    return index


def remote(src, dst, send, recv, device):
    return pltpu.make_async_remote_copy(
        src_ref=src, dst_ref=dst, send_sem=send, recv_sem=recv,
        device_id=device, device_id_type=MESH,
    )


def gather_kernel(
    tp, blocks, shards, tokens_in, gain_in, up_in, down_in, up_out, down_out, hidden_out,
    tokens, gain, up, down, loads, gath, normed, acc, xs, xr, fsend, frecv, ps, pr, ds_, dr, pds, pdr,
):
    load = [
        pltpu.make_async_copy(source, kept, loads.at[i])
        for i, (source, kept) in enumerate(
            [(gain_in, gain), (up_in, up), (down_in, down), (tokens_in, tokens)]
        )
    ]
    for copy in load:
        copy.start()
    g, f, t = lax.axis_index("gr"), lax.axis_index("fs"), lax.axis_index("tp")
    per = tp // 2
    chips = gath.shape[0]
    c, k = g * per + t // 2, lax.rem(t, 2)
    rows, width = up.shape
    half = rows // 2
    block = width // blocks
    cols = down.shape[1]

    def dev(chip, shard, core):
        return (chip // per, shard, lax.rem(chip, per) * 2 + core)

    def down_cols(chip, core):
        return pl.ds(pl.multiple_of((chip * 2 + core) * cols, cols), cols)

    barrier = pltpu.get_barrier_semaphore()
    for s in range(1, chips):
        pl.semaphore_signal(
            barrier, inc=1, device_id=dev(lax.rem(c + s, chips), f, k), device_id_type=MESH
        )
    for s in range(shards):
        for core in range(2):
            if s == 0 and core == 0:
                continue
            other = lax.rem(f + s, shards)
            core_id = lax.rem(k + core, 2)
            pl.semaphore_signal(
                barrier, inc=1, device_id=dev(c, other, core_id), device_id_type=MESH
            )

    load[0].wait()
    square = (rows, rows)
    diagonal = lax.broadcasted_iota(jnp.int32, square, 0) == lax.broadcasted_iota(jnp.int32, square, 1)
    column = jnp.sum(jnp.where(diagonal, gain[...], 0.0), axis=1, keepdims=True)
    load[1].wait()
    gath[c] = (column * up[...]).astype(jnp.bfloat16)
    load[2].wait()
    down_out[:, down_cols(c, k)] = down[...].astype(jnp.bfloat16)
    pl.semaphore_wait(barrier, chips - 1 + 2 * shards - 1)

    slices = xs.shape[2] // 2
    piece = half // slices

    def unit(chip, j, u):
        return gath.at[chip, pl.ds(u * piece, piece), pl.ds(j * block, block)]

    def up_rows(shard, core):
        return up_out.at[pl.ds(pl.multiple_of(shard * rows + core * half, half), half), :]

    def target(chip, j):
        return (chip * 2 + k) * blocks + j

    def landing(u):
        return up_out.at[pl.ds(pl.multiple_of(f * rows + u * piece, piece), piece), :]

    def forward(chip, j, u):
        to = target(chip, j)
        return remote(
            unit(chip, j, u), landing(u), fsend.at[chip, j, u], frecv.at[f],
            dev(c, to, u // slices),
        )

    def stays(chip, j, u):
        return jnp.logical_and(target(chip, j) == f, k == u // slices)

    def start_forward(chip, j, h):
        @pl.when(jnp.logical_not(stays(chip, j, h)))
        def _():
            forward(chip, j, h).start()

        @pl.when(stays(chip, j, h))
        def _():
            landing(h)[...] = unit(chip, j, h)[...]

    def exchange(s, j, h):
        return remote(
            unit(c, j, h), unit(c, j, h), xs.at[s, j, h], xr.at[s, j, h],
            dev(lax.rem(c + s, chips), f, k),
        )

    def exchanged(s, j, h):
        source = lax.rem(c + chips - s, chips)
        return remote(
            unit(source, j, h), unit(source, j, h), xs.at[s, j, h], xr.at[s, j, h], dev(c, f, k)
        )

    def down_copy(s):
        mine = down_out.at[:, down_cols(c, k)]
        return remote(mine, mine, ds_.at[s], dr.at[s], dev(lax.rem(c + s, chips), f, k))

    def down_relay(s, core):
        held = down_out.at[:, down_cols(lax.rem(c + chips - s, chips), core)]
        return remote(held, held, pds.at[s], pdr.at[s], dev(c, f, 1 - k))

    units = [(j, q + core * slices) for q in range(slices) for core in range(2) for j in range(blocks)]
    for j, h in units:
        for s in range(1, chips):
            exchange(s, j, h).start()
        start_forward(c, j, h)
    for s in range(1, chips):
        down_copy(s).start()
    down_relay(0, k).start()

    load[3].wait()
    widened = tokens[...].astype(jnp.float32)
    scale = lax.rsqrt(jnp.mean(widened * widened, axis=-1, keepdims=True) + 1e-06)
    for shard in range(shards):
        part = tokens[:, shard * rows:(shard + 1) * rows].astype(jnp.float32)
        normed[shard] = (part * scale).astype(jnp.bfloat16)

    for j, h in units:
        for s in range(1, chips):
            exchanged(s, j, h).wait_recv()
            start_forward(lax.rem(c + chips - s, chips), j, h)

    source_core = lax.rem(f // blocks, 2)
    own_stays = source_core == k

    def arrival(shard):
        return remote(
            up_rows(shard, k), up_rows(shard, k), ps.at[shard], frecv.at[shard], dev(c, f, 1 - k)
        )

    def relay(shard, core):
        held = up_rows(shard, core)
        return remote(held, held, ps.at[shard], pr.at[shard], dev(c, f, 1 - k))

    def accumulate(shard, first):
        weights = up_out[pl.ds(pl.multiple_of(shard * rows, rows), rows), :]
        product = jnp.dot(normed[shard], weights, preferred_element_type=jnp.float32)
        if first:
            acc[...] = product
        else:
            acc[...] += product

    order = [flipped(f, s, shards) for s in list(range(1, shards)) + [0]]
    for position, shard in enumerate(order):
        if position < shards - 1:
            arrival(shard).wait_recv()
        else:
            @pl.when(jnp.logical_not(own_stays))
            def _():
                arrival(shard).wait_recv()
        relay(shard, k).start()
        if position > 0:
            before = order[position - 1]
            relay(before, 1 - k).wait_recv()
            accumulate(before, position == 1)
    for s in range(1, chips):
        down_copy_in = remote(
            down_out.at[:, down_cols(lax.rem(c + chips - s, chips), k)],
            down_out.at[:, down_cols(lax.rem(c + chips - s, chips), k)],
            ds_.at[s], dr.at[s], dev(c, f, 1 - k),
        )
        down_copy_in.wait_recv()
        down_relay(s, k).start()
    relay(order[-1], 1 - k).wait_recv()
    accumulate(order[-1], False)
    hidden_out[...] = jnp.square(jnp.maximum(acc[...], 0.0)).astype(jnp.bfloat16)

    for s in range(chips):
        down_relay(s, 1 - k).wait_recv()
        down_relay(s, k).wait_send()
    for s in range(1, chips):
        down_copy(s).wait_send()
        for j, h in units:
            exchange(s, j, h).wait_send()
    for shard in order:
        relay(shard, k).wait_send()
    for s in range(chips):
        chip = lax.rem(c + s, chips)
        for j, h in units:
            @pl.when(jnp.logical_not(stays(chip, j, h)))
            def _():
                forward(chip, j, h).wait_send()


def partial_kernel(hidden, up, down, up_out, down_out, part, sems):
    copies = [
        pltpu.make_async_copy(up, up_out, sems.at[0]),
        pltpu.make_async_copy(down, down_out, sems.at[1]),
    ]
    for copy in copies:
        copy.start()
    shards, _, wide = part.shape
    for pair in range(shards // 2):
        both = jnp.dot(
            hidden[...], down[:, 2 * pair * wide:2 * (pair + 1) * wide],
            preferred_element_type=jnp.float32,
        ).astype(jnp.bfloat16)
        part[2 * pair] = both[:, :wide]
        part[2 * pair + 1] = both[:, wide:]
    for copy in copies:
        copy.wait()


def reduce_kernel(part, mixed, ybuf, zout, zbuf, ys, yr, zs, zr):
    g, f, t = lax.axis_index("gr"), lax.axis_index("fs"), lax.axis_index("tp")
    pairs = ybuf.shape[0]
    wide = mixed.shape[1]
    z, y = f // 2, lax.rem(f, 2)

    barrier = pltpu.get_barrier_semaphore()
    pl.semaphore_signal(
        barrier, inc=1, device_id=(g, z * 2 + 1 - y, t), device_id_type=MESH
    )
    for s in range(1, pairs):
        pl.semaphore_signal(
            barrier, inc=1, device_id=(g, lax.rem(z + s, pairs) * 2 + y, t), device_id_type=MESH
        )
    order = [flipped(z, s, pairs) for s in list(range(pairs - 1, 0, -1)) + [0]]

    pieces = ys.shape[1]
    span = mixed.shape[0] // pieces

    def across(pair, i):
        tokens = pl.ds(i * span, span)
        return remote(
            part.at[2 * pair + 1 - y, tokens], ybuf.at[pair, tokens], ys.at[pair, i],
            yr.at[pair, i], (g, z * 2 + 1 - y, t),
        )

    def along(pair, sender, i):
        tokens = pl.ds(i * span, span)
        return remote(
            zout.at[pair, tokens], zbuf.at[sender, tokens], zs.at[pair, i], zr.at[sender, i],
            (g, pair * 2 + y, t),
        )

    pl.semaphore_wait(barrier, pairs)
    for pair in order:
        for i in range(pieces):
            across(pair, i).start()

    def summed(pair, i):
        tokens = pl.ds(i * span, span)
        return part[2 * pair + y, tokens].astype(jnp.float32) + ybuf[pair, tokens].astype(jnp.float32)

    for pair in order[:-1]:
        for i in range(pieces):
            across(pair, i).wait_recv()
            zout[pair, pl.ds(i * span, span)] = summed(pair, i).astype(jnp.bfloat16)
            along(pair, z, i).start()
    for i in range(pieces):
        tokens = pl.ds(i * span, span)
        across(z, i).wait_recv()
        total = summed(z, i)
        for pair in order[:-1]:
            along(z, pair, i).wait_recv()
            total = total + zbuf[pair, tokens].astype(jnp.float32)
        mixed[tokens] = total.astype(jnp.bfloat16)
    for i in range(pieces):
        for pair in order:
            across(pair, i).wait_send()
        for pair in order[:-1]:
            along(pair, z, i).wait_send()


def per_device(gr, fs, tp, tokens, norm_gain, up_weight, down_weight):
    rows, width = up_weight.shape
    units, cols = down_weight.shape
    group = gr * tp
    chips = group // 2
    slices = max(1, rows // 2 // SLICE_ROWS)
    block = width * group // fs
    blocks = width // block
    count, depth = tokens.shape
    model = cols * group
    vmem = pl.BlockSpec(memory_space=pltpu.VMEM)
    hbm = pl.BlockSpec(memory_space=pltpu.HBM)
    bf16, f32 = jnp.bfloat16, jnp.float32
    dma = pltpu.SemaphoreType.DMA
    up_block, down_columns, hidden = pl.pallas_call(
        functools.partial(gather_kernel, tp, blocks, fs),
        out_shape=(
            jax.ShapeDtypeStruct((depth, block), bf16),
            jax.ShapeDtypeStruct((units, model), bf16),
            jax.ShapeDtypeStruct((count, block), bf16),
        ),
        in_specs=[hbm] * 4,
        out_specs=(vmem,) * 3,
        scratch_shapes=[
            pltpu.VMEM(tokens.shape, bf16),
            pltpu.VMEM((1, rows), f32),
            pltpu.VMEM(up_weight.shape, f32),
            pltpu.VMEM(down_weight.shape, f32),
            dma((4,)),
            pltpu.VMEM((chips, rows, width), bf16),
            pltpu.VMEM((fs, count, rows), bf16),
            pltpu.VMEM((count, block), f32),
            *[dma((chips, blocks, 2 * slices)) for _ in range(3)], dma((fs,)),
            dma((fs,)), dma((fs,)),
            dma((chips,)), dma((chips,)), dma((chips,)), dma((chips,)),
        ],
        compiler_params=pltpu.CompilerParams(
            collective_id=0, has_side_effects=True, vmem_limit_bytes=GATHER_VMEM * MIB
        ),
        cost_estimate=pl.CostEstimate(
            flops=2 * count * depth * block, bytes_accessed=160 * MIB, transcendentals=0
        ),
    )(*[pltpu.with_memory_space_constraint(x, pltpu.HBM) for x in (tokens, norm_gain[None, :], up_weight, down_weight)])
    pairs = fs // 2
    wide = model // fs
    up_block, down_columns, part = pl.pallas_call(
        partial_kernel,
        out_shape=(
            jax.ShapeDtypeStruct(up_block.shape, bf16),
            jax.ShapeDtypeStruct(down_columns.shape, bf16),
            jax.ShapeDtypeStruct((fs, count, wide), bf16),
        ),
        in_specs=[vmem] * 3,
        out_specs=(hbm, hbm, vmem),
        scratch_shapes=[dma((2,))],
        compiler_params=pltpu.CompilerParams(vmem_limit_bytes=PARTIAL_VMEM * MIB),
        cost_estimate=pl.CostEstimate(
            flops=2 * count * units * model, bytes_accessed=16 * MIB, transcendentals=0
        ),
    )(hidden, up_block, down_columns)
    mixed = pl.pallas_call(
        reduce_kernel,
        out_shape=jax.ShapeDtypeStruct((count, wide), bf16),
        in_specs=[vmem],
        out_specs=vmem,
        scratch_shapes=[
            pltpu.VMEM((pairs, count, wide), bf16),
            pltpu.VMEM((pairs, count, wide), bf16),
            pltpu.VMEM((pairs, count, wide), bf16),
            *[dma((pairs, PIECES)) for _ in range(4)],
        ],
        compiler_params=pltpu.CompilerParams(
            collective_id=1, has_side_effects=True, vmem_limit_bytes=REDUCE_VMEM * MIB
        ),
        cost_estimate=pl.CostEstimate(
            flops=count * model, bytes_accessed=100 * MIB, transcendentals=0
        ),
    )(part)
    return (up_block, down_columns, mixed)


def solution(mesh):
    in_specs = (P(("gr", "tp"), None), P("fs"), P("fs", ("gr", "tp")), P("fs", ("gr", "tp")))
    out_specs = (P(None, "fs"), P("fs", None), P(("gr", "tp"), "fs"))
    body = functools.partial(per_device, mesh.shape["gr"], mesh.shape["fs"], mesh.shape["tp"])
    return jax.shard_map(
        body, mesh=mesh, in_specs=in_specs, out_specs=out_specs, check_vma=False
    )
```

```python
import functools

import jax
import jax.numpy as jnp
from jax import lax
from jax.experimental import pallas as pl
from jax.experimental.pallas import tpu as pltpu
from jax.sharding import PartitionSpec as P

MESH = pl.DeviceIdType.MESH
MIB = 1024 * 1024
GATHER_VMEM = 32
PARTIAL_VMEM = 20
REDUCE_VMEM = 20
SLICE_ROWS = 32
PIECES = 4


def flipped(index, step, count):
    if count & (count - 1):
        return lax.rem(index + step, count)
    bit = 1
    while bit < count:
        if step & bit:
            index = index + (1 - 2 * lax.rem(index // bit, 2)) * bit
        bit *= 2
    return index


def remote(src, dst, send, recv, device):
    return pltpu.make_async_remote_copy(
        src_ref=src, dst_ref=dst, send_sem=send, recv_sem=recv,
        device_id=device, device_id_type=MESH,
    )


def gather_kernel(
    tp, blocks, shards, tokens_in, gain_in, up_in, down_in, up_out, down_out, hidden_out,
    tokens, gain, up, down, loads, gath, normed, acc, xs, xr, fsend, frecv, ps, pr, ds_, dr, pds, pdr,
):
    load = [
        pltpu.make_async_copy(source, kept, loads.at[i])
        for i, (source, kept) in enumerate(
            [(gain_in, gain), (up_in, up), (down_in, down), (tokens_in, tokens)]
        )
    ]
    for copy in load:
        copy.start()
    g, f, t = lax.axis_index("gr"), lax.axis_index("fs"), lax.axis_index("tp")
    per = tp // 2
    chips = gath.shape[0]
    c, k = g * per + t // 2, lax.rem(t, 2)
    rows, width = up.shape
    half = rows // 2
    block = width // blocks
    cols = down.shape[1]

    def dev(chip, shard, core):
        return (chip // per, shard, lax.rem(chip, per) * 2 + core)

    def down_cols(chip, core):
        return pl.ds(pl.multiple_of((chip * 2 + core) * cols, cols), cols)

    barrier = pltpu.get_barrier_semaphore()
    for s in range(1, chips):
        pl.semaphore_signal(
            barrier, inc=1, device_id=dev(lax.rem(c + s, chips), f, k), device_id_type=MESH
        )
    for s in range(shards):
        for core in range(2):
            if s == 0 and core == 0:
                continue
            other = lax.rem(f + s, shards)
            core_id = lax.rem(k + core, 2)
            pl.semaphore_signal(
                barrier, inc=1, device_id=dev(c, other, core_id), device_id_type=MESH
            )

    load[0].wait()
    square = (rows, rows)
    diagonal = lax.broadcasted_iota(jnp.int32, square, 0) == lax.broadcasted_iota(jnp.int32, square, 1)
    column = jnp.sum(jnp.where(diagonal, gain[...], 0.0), axis=1, keepdims=True)
    load[1].wait()
    gath[c] = (column * up[...]).astype(jnp.bfloat16)
    load[2].wait()
    down_out[:, down_cols(c, k)] = down[...].astype(jnp.bfloat16)
    pl.semaphore_wait(barrier, chips - 1 + 2 * shards - 1)

    slices = xs.shape[2] // 2
    piece = half // slices

    def unit(chip, j, u):
        return gath.at[chip, pl.ds(u * piece, piece), pl.ds(j * block, block)]

    def up_rows(shard, core):
        return up_out.at[pl.ds(pl.multiple_of(shard * rows + core * half, half), half), :]

    def target(chip, j):
        return (chip * 2 + k) * blocks + j

    def landing(u):
        return up_out.at[pl.ds(pl.multiple_of(f * rows + u * piece, piece), piece), :]

    def forward(chip, j, u):
        to = target(chip, j)
        return remote(
            unit(chip, j, u), landing(u), fsend.at[chip, j, u], frecv.at[f],
            dev(c, to, u // slices),
        )

    def stays(chip, j, u):
        return jnp.logical_and(target(chip, j) == f, k == u // slices)

    def start_forward(chip, j, h):
        @pl.when(jnp.logical_not(stays(chip, j, h)))
        def _():
            forward(chip, j, h).start()

        @pl.when(stays(chip, j, h))
        def _():
            landing(h)[...] = unit(chip, j, h)[...]

    def exchange(s, j, h):
        return remote(
            unit(c, j, h), unit(c, j, h), xs.at[s, j, h], xr.at[s, j, h],
            dev(lax.rem(c + s, chips), f, k),
        )

    def exchanged(s, j, h):
        source = lax.rem(c + chips - s, chips)
        return remote(
            unit(source, j, h), unit(source, j, h), xs.at[s, j, h], xr.at[s, j, h], dev(c, f, k)
        )

    def down_copy(s):
        mine = down_out.at[:, down_cols(c, k)]
        return remote(mine, mine, ds_.at[s], dr.at[s], dev(lax.rem(c + s, chips), f, k))

    def down_relay(s, core):
        held = down_out.at[:, down_cols(lax.rem(c + chips - s, chips), core)]
        return remote(held, held, pds.at[s], pdr.at[s], dev(c, f, 1 - k))

    units = [(j, q + core * slices) for q in range(slices) for core in range(2) for j in range(blocks)]
    for j, h in units:
        for s in range(1, chips):
            exchange(s, j, h).start()
        start_forward(c, j, h)
    for s in range(1, chips):
        down_copy(s).start()
    down_relay(0, k).start()

    load[3].wait()
    widened = tokens[...].astype(jnp.float32)
    scale = lax.rsqrt(jnp.mean(widened * widened, axis=-1, keepdims=True) + 1e-06)
    for shard in range(shards):
        part = tokens[:, shard * rows:(shard + 1) * rows].astype(jnp.float32)
        normed[shard] = (part * scale).astype(jnp.bfloat16)

    for j, h in units:
        for s in range(1, chips):
            exchanged(s, j, h).wait_recv()
            start_forward(lax.rem(c + chips - s, chips), j, h)

    source_core = lax.rem(f // blocks, 2)
    own_stays = source_core == k

    def arrival(shard):
        return remote(
            up_rows(shard, k), up_rows(shard, k), ps.at[shard], frecv.at[shard], dev(c, f, 1 - k)
        )

    def relay(shard, core):
        held = up_rows(shard, core)
        return remote(held, held, ps.at[shard], pr.at[shard], dev(c, f, 1 - k))

    def accumulate(shard, first):
        weights = up_out[pl.ds(pl.multiple_of(shard * rows, rows), rows), :]
        product = jnp.dot(normed[shard], weights, preferred_element_type=jnp.float32)
        if first:
            acc[...] = product
        else:
            acc[...] += product

    order = [flipped(f, s, shards) for s in list(range(1, shards)) + [0]]
    for position, shard in enumerate(order):
        if position < shards - 1:
            arrival(shard).wait_recv()
        else:
            @pl.when(jnp.logical_not(own_stays))
            def _():
                arrival(shard).wait_recv()
        relay(shard, k).start()
        if position > 0:
            before = order[position - 1]
            relay(before, 1 - k).wait_recv()
            accumulate(before, position == 1)
    for s in range(1, chips):
        down_copy_in = remote(
            down_out.at[:, down_cols(lax.rem(c + chips - s, chips), k)],
            down_out.at[:, down_cols(lax.rem(c + chips - s, chips), k)],
            ds_.at[s], dr.at[s], dev(c, f, 1 - k),
        )
        down_copy_in.wait_recv()
        down_relay(s, k).start()
    relay(order[-1], 1 - k).wait_recv()
    accumulate(order[-1], False)
    hidden_out[...] = jnp.square(jnp.maximum(acc[...], 0.0)).astype(jnp.bfloat16)

    for s in range(chips):
        down_relay(s, 1 - k).wait_recv()
        down_relay(s, k).wait_send()
    for s in range(1, chips):
        down_copy(s).wait_send()
        for j, h in units:
            exchange(s, j, h).wait_send()
    for shard in order:
        relay(shard, k).wait_send()
    for s in range(chips):
        chip = lax.rem(c + s, chips)
        for j, h in units:
            @pl.when(jnp.logical_not(stays(chip, j, h)))
            def _():
                forward(chip, j, h).wait_send()


def partial_kernel(hidden, up, down, up_out, down_out, part, sems):
    copies = [
        pltpu.make_async_copy(up, up_out, sems.at[0]),
        pltpu.make_async_copy(down, down_out, sems.at[1]),
    ]
    for copy in copies:
        copy.start()
    shards, _, wide = part.shape
    for pair in range(shards // 2):
        both = jnp.dot(
            hidden[...], down[:, 2 * pair * wide:2 * (pair + 1) * wide],
            preferred_element_type=jnp.float32,
        ).astype(jnp.bfloat16)
        part[2 * pair] = both[:, :wide]
        part[2 * pair + 1] = both[:, wide:]
    for copy in copies:
        copy.wait()


def reduce_kernel(part, mixed, ybuf, zout, zbuf, gbuf, ys, yr, zs, zr, gr_sem):
    g, f, t = lax.axis_index("gr"), lax.axis_index("fs"), lax.axis_index("tp")
    pairs, pieces = ys.shape
    side = pairs // 2
    span = mixed.shape[0] // pieces
    z, y = f // 2, lax.rem(f, 2)
    upper, odd = z // side, lax.rem(z, 2)
    is_gate = lax.rem(odd + upper, 2) == 1
    mate = z + 1 - 2 * odd
    far = [(1 - upper) * side + i for i in range(side)]
    near = [upper * side + lax.rem(lax.rem(z, side) + s, side) for s in range(1, side)]
    far_gates = [(1 - upper) * side + 2 * i + upper for i in range(side // 2)]

    barrier = pltpu.get_barrier_semaphore()
    pl.semaphore_signal(
        barrier, inc=1, device_id=(g, z * 2 + 1 - y, t), device_id_type=MESH
    )
    for s in range(1, pairs):
        pl.semaphore_signal(
            barrier, inc=1, device_id=(g, lax.rem(z + s, pairs) * 2 + y, t), device_id_type=MESH
        )
    rows = [pl.ds(i * span, span) for i in range(pieces)]

    def across(pair, i):
        return remote(
            part.at[2 * pair + 1 - y, rows[i]], ybuf.at[pair, rows[i]], ys.at[pair, i],
            yr.at[pair, i], (g, z * 2 + 1 - y, t),
        )

    def along(pair, sender, i):
        return remote(
            zout.at[pair, rows[i]], zbuf.at[sender, rows[i]], zs.at[pair, i], zr.at[sender, i],
            (g, pair * 2 + y, t),
        )

    def to_mate(pair, i):
        return remote(
            zout.at[pair, rows[i]], gbuf.at[pair, rows[i]], zs.at[pair, i], gr_sem.at[pair, i],
            (g, mate * 2 + y, t),
        )

    pl.semaphore_wait(barrier, pairs)
    for pair in far + near + [z]:
        for i in range(pieces):
            across(pair, i).start()

    def summed(pair, i):
        return part[2 * pair + y, rows[i]].astype(jnp.float32) + ybuf[pair, rows[i]].astype(jnp.float32)

    @pl.when(is_gate)
    def _():
        for pair in far:
            for i in range(pieces):
                across(pair, i).wait_recv()
                to_mate(pair, i).wait_recv()
                total = summed(pair, i) + gbuf[pair, rows[i]].astype(jnp.float32)
                zout[pair, rows[i]] = total.astype(jnp.bfloat16)
                along(pair, z, i).start()

    @pl.when(jnp.logical_not(is_gate))
    def _():
        for pair in far:
            for i in range(pieces):
                across(pair, i).wait_recv()
                zout[pair, rows[i]] = summed(pair, i).astype(jnp.bfloat16)
                to_mate(pair, i).start()

    for pair in near:
        for i in range(pieces):
            across(pair, i).wait_recv()
            zout[pair, rows[i]] = summed(pair, i).astype(jnp.bfloat16)
            along(pair, z, i).start()
    for i in range(pieces):
        across(z, i).wait_recv()
        total = summed(z, i)
        for sender in far_gates + near:
            along(z, sender, i).wait_recv()
            total = total + zbuf[sender, rows[i]].astype(jnp.float32)
        mixed[rows[i]] = total.astype(jnp.bfloat16)
    for i in range(pieces):
        for pair in far + near + [z]:
            across(pair, i).wait_send()
        for pair in far + near:
            along(pair, z, i).wait_send()


def per_device(gr, fs, tp, tokens, norm_gain, up_weight, down_weight):
    rows, width = up_weight.shape
    units, cols = down_weight.shape
    group = gr * tp
    chips = group // 2
    slices = max(1, rows // 2 // SLICE_ROWS)
    block = width * group // fs
    blocks = width // block
    count, depth = tokens.shape
    model = cols * group
    vmem = pl.BlockSpec(memory_space=pltpu.VMEM)
    hbm = pl.BlockSpec(memory_space=pltpu.HBM)
    bf16, f32 = jnp.bfloat16, jnp.float32
    dma = pltpu.SemaphoreType.DMA
    up_block, down_columns, hidden = pl.pallas_call(
        functools.partial(gather_kernel, tp, blocks, fs),
        out_shape=(
            jax.ShapeDtypeStruct((depth, block), bf16),
            jax.ShapeDtypeStruct((units, model), bf16),
            jax.ShapeDtypeStruct((count, block), bf16),
        ),
        in_specs=[hbm] * 4,
        out_specs=(vmem,) * 3,
        scratch_shapes=[
            pltpu.VMEM(tokens.shape, bf16),
            pltpu.VMEM((1, rows), f32),
            pltpu.VMEM(up_weight.shape, f32),
            pltpu.VMEM(down_weight.shape, f32),
            dma((4,)),
            pltpu.VMEM((chips, rows, width), bf16),
            pltpu.VMEM((fs, count, rows), bf16),
            pltpu.VMEM((count, block), f32),
            *[dma((chips, blocks, 2 * slices)) for _ in range(3)], dma((fs,)),
            dma((fs,)), dma((fs,)),
            dma((chips,)), dma((chips,)), dma((chips,)), dma((chips,)),
        ],
        compiler_params=pltpu.CompilerParams(
            collective_id=0, has_side_effects=True, vmem_limit_bytes=GATHER_VMEM * MIB
        ),
        cost_estimate=pl.CostEstimate(
            flops=2 * count * depth * block, bytes_accessed=160 * MIB, transcendentals=0
        ),
    )(*[pltpu.with_memory_space_constraint(x, pltpu.HBM) for x in (tokens, norm_gain[None, :], up_weight, down_weight)])
    pairs = fs // 2
    wide = model // fs
    up_block, down_columns, part = pl.pallas_call(
        partial_kernel,
        out_shape=(
            jax.ShapeDtypeStruct(up_block.shape, bf16),
            jax.ShapeDtypeStruct(down_columns.shape, bf16),
            jax.ShapeDtypeStruct((fs, count, wide), bf16),
        ),
        in_specs=[vmem] * 3,
        out_specs=(hbm, hbm, vmem),
        scratch_shapes=[dma((2,))],
        compiler_params=pltpu.CompilerParams(vmem_limit_bytes=PARTIAL_VMEM * MIB),
        cost_estimate=pl.CostEstimate(
            flops=2 * count * units * model, bytes_accessed=16 * MIB, transcendentals=0
        ),
    )(hidden, up_block, down_columns)
    mixed = pl.pallas_call(
        reduce_kernel,
        out_shape=jax.ShapeDtypeStruct((count, wide), bf16),
        in_specs=[vmem],
        out_specs=vmem,
        scratch_shapes=[
            pltpu.VMEM((pairs, count, wide), bf16),
            pltpu.VMEM((pairs, count, wide), bf16),
            pltpu.VMEM((pairs, count, wide), bf16),
            pltpu.VMEM((pairs, count, wide), bf16),
            *[dma((pairs, PIECES)) for _ in range(5)],
        ],
        compiler_params=pltpu.CompilerParams(
            collective_id=1, has_side_effects=True, vmem_limit_bytes=REDUCE_VMEM * MIB
        ),
        cost_estimate=pl.CostEstimate(
            flops=count * model, bytes_accessed=100 * MIB, transcendentals=0
        ),
    )(part)
    return (up_block, down_columns, mixed)


def solution(mesh):
    in_specs = (P(("gr", "tp"), None), P("fs"), P("fs", ("gr", "tp")), P("fs", ("gr", "tp")))
    out_specs = (P(None, "fs"), P("fs", None), P(("gr", "tp"), "fs"))
    body = functools.partial(per_device, mesh.shape["gr"], mesh.shape["fs"], mesh.shape["tp"])
    return jax.shard_map(
        body, mesh=mesh, in_specs=in_specs, out_specs=out_specs, check_vma=False
    )
```

```python
import functools

import jax
import jax.numpy as jnp
from jax import lax
from jax.experimental import pallas as pl
from jax.experimental.pallas import tpu as pltpu
from jax.sharding import PartitionSpec as P

MESH = pl.DeviceIdType.MESH
MIB = 1024 * 1024
GATHER_VMEM = 32
PARTIAL_VMEM = 20
REDUCE_VMEM = 20
SLICE_ROWS = 32
PIECES = 4


def flipped(index, step, count):
    if count & (count - 1):
        return lax.rem(index + step, count)
    bit = 1
    while bit < count:
        if step & bit:
            index = index + (1 - 2 * lax.rem(index // bit, 2)) * bit
        bit *= 2
    return index


def remote(src, dst, send, recv, device):
    return pltpu.make_async_remote_copy(
        src_ref=src, dst_ref=dst, send_sem=send, recv_sem=recv,
        device_id=device, device_id_type=MESH,
    )


def gather_kernel(
    tp, blocks, shards, tokens_in, gain_in, up_in, down_in, up_out, down_out, hidden_out,
    tokens, gain, up, down, loads, gath, normed, acc, xs, xr, fsend, frecv, ps, pr, ds_, dr, pds, pdr,
):
    load = [
        pltpu.make_async_copy(source, kept, loads.at[i])
        for i, (source, kept) in enumerate(
            [(gain_in, gain), (up_in, up), (down_in, down), (tokens_in, tokens)]
        )
    ]
    for copy in load:
        copy.start()
    g, f, t = lax.axis_index("gr"), lax.axis_index("fs"), lax.axis_index("tp")
    per = tp // 2
    chips = gath.shape[0]
    c, k = g * per + t // 2, lax.rem(t, 2)
    rows, width = up.shape
    half = rows // 2
    block = width // blocks
    cols = down.shape[1]

    def dev(chip, shard, core):
        return (chip // per, shard, lax.rem(chip, per) * 2 + core)

    def down_cols(chip, core):
        return pl.ds(pl.multiple_of((chip * 2 + core) * cols, cols), cols)

    barrier = pltpu.get_barrier_semaphore()
    for s in range(1, chips):
        pl.semaphore_signal(
            barrier, inc=1, device_id=dev(lax.rem(c + s, chips), f, k), device_id_type=MESH
        )
    for s in range(shards):
        for core in range(2):
            if s == 0 and core == 0:
                continue
            other = lax.rem(f + s, shards)
            core_id = lax.rem(k + core, 2)
            pl.semaphore_signal(
                barrier, inc=1, device_id=dev(c, other, core_id), device_id_type=MESH
            )

    load[0].wait()
    square = (rows, rows)
    diagonal = lax.broadcasted_iota(jnp.int32, square, 0) == lax.broadcasted_iota(jnp.int32, square, 1)
    column = jnp.sum(jnp.where(diagonal, gain[...], 0.0), axis=1, keepdims=True)
    load[1].wait()
    gath[c] = (column * up[...]).astype(jnp.bfloat16)
    pl.semaphore_wait(barrier, chips - 1 + 2 * shards - 1)

    slices = xs.shape[2] // 2
    piece = half // slices

    def unit(chip, j, u):
        return gath.at[chip, pl.ds(u * piece, piece), pl.ds(j * block, block)]

    def up_rows(shard, core):
        return up_out.at[pl.ds(pl.multiple_of(shard * rows + core * half, half), half), :]

    def target(chip, j):
        return (chip * 2 + k) * blocks + j

    def landing(u):
        return up_out.at[pl.ds(pl.multiple_of(f * rows + u * piece, piece), piece), :]

    def forward(chip, j, u):
        to = target(chip, j)
        return remote(
            unit(chip, j, u), landing(u), fsend.at[chip, j, u], frecv.at[f],
            dev(c, to, u // slices),
        )

    def stays(chip, j, u):
        return jnp.logical_and(target(chip, j) == f, k == u // slices)

    def start_forward(chip, j, h):
        @pl.when(jnp.logical_not(stays(chip, j, h)))
        def _():
            forward(chip, j, h).start()

        @pl.when(stays(chip, j, h))
        def _():
            landing(h)[...] = unit(chip, j, h)[...]

    def exchange(s, j, h):
        return remote(
            unit(c, j, h), unit(c, j, h), xs.at[s, j, h], xr.at[s, j, h],
            dev(lax.rem(c + s, chips), f, k),
        )

    def exchanged(s, j, h):
        source = lax.rem(c + chips - s, chips)
        return remote(
            unit(source, j, h), unit(source, j, h), xs.at[s, j, h], xr.at[s, j, h], dev(c, f, k)
        )

    def down_copy(s):
        mine = down_out.at[:, down_cols(c, k)]
        return remote(mine, mine, ds_.at[s], dr.at[s], dev(lax.rem(c + s, chips), f, k))

    def down_relay(s, core):
        held = down_out.at[:, down_cols(lax.rem(c + chips - s, chips), core)]
        return remote(held, held, pds.at[s], pdr.at[s], dev(c, f, 1 - k))

    units = [(j, q + core * slices) for q in range(slices) for core in range(2) for j in range(blocks)]
    for j, h in units:
        for s in range(1, chips):
            exchange(s, j, h).start()
        start_forward(c, j, h)
    for index, (j, h) in enumerate(units):
        if index == len(units) // 2:
            load[2].wait()
            down_out[:, down_cols(c, k)] = down[...].astype(jnp.bfloat16)
        if index == 3 * len(units) // 4:
            for s in range(1, chips):
                down_copy(s).start()
            down_relay(0, k).start()
        for s in range(1, chips):
            exchanged(s, j, h).wait_recv()
            start_forward(lax.rem(c + chips - s, chips), j, h)

    load[3].wait()
    widened = tokens[...].astype(jnp.float32)
    scale = lax.rsqrt(jnp.mean(widened * widened, axis=-1, keepdims=True) + 1e-06)
    for shard in range(shards):
        part = tokens[:, shard * rows:(shard + 1) * rows].astype(jnp.float32)
        normed[shard] = (part * scale).astype(jnp.bfloat16)

    source_core = lax.rem(f // blocks, 2)
    own_stays = source_core == k

    def arrival(shard):
        return remote(
            up_rows(shard, k), up_rows(shard, k), ps.at[shard], frecv.at[shard], dev(c, f, 1 - k)
        )

    def relay(shard, core):
        held = up_rows(shard, core)
        return remote(held, held, ps.at[shard], pr.at[shard], dev(c, f, 1 - k))

    def accumulate(shard, first):
        weights = up_out[pl.ds(pl.multiple_of(shard * rows, rows), rows), :]
        product = jnp.dot(normed[shard], weights, preferred_element_type=jnp.float32)
        if first:
            acc[...] = product
        else:
            acc[...] += product

    order = [flipped(f, s, shards) for s in list(range(1, shards)) + [0]]
    for position, shard in enumerate(order):
        if position < shards - 1:
            arrival(shard).wait_recv()
        else:
            @pl.when(jnp.logical_not(own_stays))
            def _():
                arrival(shard).wait_recv()
        relay(shard, k).start()
        if position > 0:
            before = order[position - 1]
            relay(before, 1 - k).wait_recv()
            accumulate(before, position == 1)
    for s in range(1, chips):
        down_copy_in = remote(
            down_out.at[:, down_cols(lax.rem(c + chips - s, chips), k)],
            down_out.at[:, down_cols(lax.rem(c + chips - s, chips), k)],
            ds_.at[s], dr.at[s], dev(c, f, 1 - k),
        )
        down_copy_in.wait_recv()
        down_relay(s, k).start()
    relay(order[-1], 1 - k).wait_recv()
    accumulate(order[-1], False)
    hidden_out[...] = jnp.square(jnp.maximum(acc[...], 0.0)).astype(jnp.bfloat16)

    for s in range(chips):
        down_relay(s, 1 - k).wait_recv()
        down_relay(s, k).wait_send()
    for s in range(1, chips):
        down_copy(s).wait_send()
        for j, h in units:
            exchange(s, j, h).wait_send()
    for shard in order:
        relay(shard, k).wait_send()
    for s in range(chips):
        chip = lax.rem(c + s, chips)
        for j, h in units:
            @pl.when(jnp.logical_not(stays(chip, j, h)))
            def _():
                forward(chip, j, h).wait_send()


def partial_kernel(hidden, up, down, up_out, down_out, part, sems):
    copies = [
        pltpu.make_async_copy(up, up_out, sems.at[0]),
        pltpu.make_async_copy(down, down_out, sems.at[1]),
    ]
    for copy in copies:
        copy.start()
    shards, _, wide = part.shape
    for pair in range(shards // 2):
        both = jnp.dot(
            hidden[...], down[:, 2 * pair * wide:2 * (pair + 1) * wide],
            preferred_element_type=jnp.float32,
        ).astype(jnp.bfloat16)
        part[2 * pair] = both[:, :wide]
        part[2 * pair + 1] = both[:, wide:]
    for copy in copies:
        copy.wait()


def reduce_kernel(part, mixed, ybuf, zout, zbuf, gbuf, ys, yr, zs, zr, gr_sem):
    g, f, t = lax.axis_index("gr"), lax.axis_index("fs"), lax.axis_index("tp")
    pairs, pieces = ys.shape
    side = pairs // 2
    span = mixed.shape[0] // pieces
    z, y = f // 2, lax.rem(f, 2)
    upper, odd = z // side, lax.rem(z, 2)
    is_gate = lax.rem(odd + upper, 2) == 1
    mate = z + 1 - 2 * odd
    far = [(1 - upper) * side + i for i in range(side)]
    near = [upper * side + lax.rem(lax.rem(z, side) + s, side) for s in range(1, side)]
    far_gates = [(1 - upper) * side + 2 * i + upper for i in range(side // 2)]

    barrier = pltpu.get_barrier_semaphore()
    pl.semaphore_signal(
        barrier, inc=1, device_id=(g, z * 2 + 1 - y, t), device_id_type=MESH
    )
    for s in range(1, pairs):
        pl.semaphore_signal(
            barrier, inc=1, device_id=(g, lax.rem(z + s, pairs) * 2 + y, t), device_id_type=MESH
        )
    rows = [pl.ds(i * span, span) for i in range(pieces)]

    def across(pair, i):
        return remote(
            part.at[2 * pair + 1 - y, rows[i]], ybuf.at[pair, rows[i]], ys.at[pair, i],
            yr.at[pair, i], (g, z * 2 + 1 - y, t),
        )

    def along(pair, sender, i):
        return remote(
            zout.at[pair, rows[i]], zbuf.at[sender, rows[i]], zs.at[pair, i], zr.at[sender, i],
            (g, pair * 2 + y, t),
        )

    def to_mate(pair, i):
        return remote(
            zout.at[pair, rows[i]], gbuf.at[pair, rows[i]], zs.at[pair, i], gr_sem.at[pair, i],
            (g, mate * 2 + y, t),
        )

    pl.semaphore_wait(barrier, pairs)
    for pair in far + near + [z]:
        for i in range(pieces):
            across(pair, i).start()

    def summed(pair, i):
        return part[2 * pair + y, rows[i]].astype(jnp.float32) + ybuf[pair, rows[i]].astype(jnp.float32)

    @pl.when(is_gate)
    def _():
        for pair in far:
            for i in range(pieces):
                across(pair, i).wait_recv()
                to_mate(pair, i).wait_recv()
                total = summed(pair, i) + gbuf[pair, rows[i]].astype(jnp.float32)
                zout[pair, rows[i]] = total.astype(jnp.bfloat16)
                along(pair, z, i).start()

    @pl.when(jnp.logical_not(is_gate))
    def _():
        for pair in far:
            for i in range(pieces):
                across(pair, i).wait_recv()
                zout[pair, rows[i]] = summed(pair, i).astype(jnp.bfloat16)
                to_mate(pair, i).start()

    for pair in near:
        for i in range(pieces):
            across(pair, i).wait_recv()
            zout[pair, rows[i]] = summed(pair, i).astype(jnp.bfloat16)
            along(pair, z, i).start()
    for i in range(pieces):
        across(z, i).wait_recv()
        total = summed(z, i)
        for sender in far_gates + near:
            along(z, sender, i).wait_recv()
            total = total + zbuf[sender, rows[i]].astype(jnp.float32)
        mixed[rows[i]] = total.astype(jnp.bfloat16)
    for i in range(pieces):
        for pair in far + near + [z]:
            across(pair, i).wait_send()
        for pair in far + near:
            along(pair, z, i).wait_send()


def per_device(gr, fs, tp, tokens, norm_gain, up_weight, down_weight):
    rows, width = up_weight.shape
    units, cols = down_weight.shape
    group = gr * tp
    chips = group // 2
    slices = max(1, rows // 2 // SLICE_ROWS)
    block = width * group // fs
    blocks = width // block
    count, depth = tokens.shape
    model = cols * group
    vmem = pl.BlockSpec(memory_space=pltpu.VMEM)
    hbm = pl.BlockSpec(memory_space=pltpu.HBM)
    bf16, f32 = jnp.bfloat16, jnp.float32
    dma = pltpu.SemaphoreType.DMA
    up_block, down_columns, hidden = pl.pallas_call(
        functools.partial(gather_kernel, tp, blocks, fs),
        out_shape=(
            jax.ShapeDtypeStruct((depth, block), bf16),
            jax.ShapeDtypeStruct((units, model), bf16),
            jax.ShapeDtypeStruct((count, block), bf16),
        ),
        in_specs=[hbm] * 4,
        out_specs=(vmem,) * 3,
        scratch_shapes=[
            pltpu.VMEM(tokens.shape, bf16),
            pltpu.VMEM((1, rows), f32),
            pltpu.VMEM(up_weight.shape, f32),
            pltpu.VMEM(down_weight.shape, f32),
            dma((4,)),
            pltpu.VMEM((chips, rows, width), bf16),
            pltpu.VMEM((fs, count, rows), bf16),
            pltpu.VMEM((count, block), f32),
            *[dma((chips, blocks, 2 * slices)) for _ in range(3)], dma((fs,)),
            dma((fs,)), dma((fs,)),
            dma((chips,)), dma((chips,)), dma((chips,)), dma((chips,)),
        ],
        compiler_params=pltpu.CompilerParams(
            collective_id=0, has_side_effects=True, vmem_limit_bytes=GATHER_VMEM * MIB
        ),
        cost_estimate=pl.CostEstimate(
            flops=2 * count * depth * block, bytes_accessed=160 * MIB, transcendentals=0
        ),
    )(*[pltpu.with_memory_space_constraint(x, pltpu.HBM) for x in (tokens, norm_gain[None, :], up_weight, down_weight)])
    pairs = fs // 2
    wide = model // fs
    up_block, down_columns, part = pl.pallas_call(
        partial_kernel,
        out_shape=(
            jax.ShapeDtypeStruct(up_block.shape, bf16),
            jax.ShapeDtypeStruct(down_columns.shape, bf16),
            jax.ShapeDtypeStruct((fs, count, wide), bf16),
        ),
        in_specs=[vmem] * 3,
        out_specs=(hbm, hbm, vmem),
        scratch_shapes=[dma((2,))],
        compiler_params=pltpu.CompilerParams(vmem_limit_bytes=PARTIAL_VMEM * MIB),
        cost_estimate=pl.CostEstimate(
            flops=2 * count * units * model, bytes_accessed=16 * MIB, transcendentals=0
        ),
    )(hidden, up_block, down_columns)
    mixed = pl.pallas_call(
        reduce_kernel,
        out_shape=jax.ShapeDtypeStruct((count, wide), bf16),
        in_specs=[vmem],
        out_specs=vmem,
        scratch_shapes=[
            pltpu.VMEM((pairs, count, wide), bf16),
            pltpu.VMEM((pairs, count, wide), bf16),
            pltpu.VMEM((pairs, count, wide), bf16),
            pltpu.VMEM((pairs, count, wide), bf16),
            *[dma((pairs, PIECES)) for _ in range(5)],
        ],
        compiler_params=pltpu.CompilerParams(
            collective_id=1, has_side_effects=True, vmem_limit_bytes=REDUCE_VMEM * MIB
        ),
        cost_estimate=pl.CostEstimate(
            flops=count * model, bytes_accessed=100 * MIB, transcendentals=0
        ),
    )(part)
    return (up_block, down_columns, mixed)


def solution(mesh):
    in_specs = (P(("gr", "tp"), None), P("fs"), P("fs", ("gr", "tp")), P("fs", ("gr", "tp")))
    out_specs = (P(None, "fs"), P("fs", None), P(("gr", "tp"), "fs"))
    body = functools.partial(per_device, mesh.shape["gr"], mesh.shape["fs"], mesh.shape["tp"])
    return jax.shard_map(
        body, mesh=mesh, in_specs=in_specs, out_specs=out_specs, check_vma=False
    )
```
